256 devices in a mesh: dp: 4 (over x), kv: 32 (over z, y), tp: 2 (over core).
Axes of the slice: x: 4, y: 4, z: 8, core: 2. Of those that a mesh axis runs over, the one named last changes fastest.
Arguments:
- tokens: bfloat16 [4, 8192, 2048], P('dp', 'kv'), may hold values from -28 to 28, as said below
- query_weight: bfloat16 [2048, 768], P(None, 'tp'), may hold values from -0.125 to 0.125
- key_weight: bfloat16 [2048, 256], P(None, 'tp'), may hold values from -0.125 to 0.125
- value_weight: bfloat16 [2048, 256], P(None, 'tp'), may hold values from -0.125 to 0.125
- gate_weight: bfloat16 [2048, 24], replicated, may hold values from -0.125 to 0.125
- compress_weight: float32 [2, 32, 64], replicated, may hold values from -1 to 1
- out_weight: bfloat16 [768, 2048], P('tp'), may hold values from -0.21875 to 0.21875
- out_gain: float32 [2048], replicated, may hold values from 0.1 to 1.9
- chosen: int32 [4, 256, 16], P('dp', 'kv'), may hold values from -1 to 255, as said below
Outputs:
- output: float32 [4, 8192, 2048], P('dp', ('kv', 'tp'))
The draws below stay inside these ranges and needn't reach their ends.
Inputs may be any that keep to these rules, and one draw needn't show every extreme that they name: `chosen`: row q of a sequence lists distinct blocks; its first entry is q itself; the others are -1 or blocks held by an earlier index of kv (block index // 8). Over the rows of one kv index, at most 2 distinct blocks come from any other single index, and every index past the first reads exactly 2 blocks of the first index, among them block 0. `tokens`: finite activations; some rows are much larger than others in some draws.
All inputs are finite; a program needn't handle non-finite values.
Results may differ from the reference program's by a relative error of at most 0.02.
The reference program's roundings to bfloat16 on the way count: a program that leaves them out, or rounds other values in their place, can miss the bound.
Values may be sent and summed in bfloat16 or wider, within the bound.
No kernel may reach another device: no remote copies, remote signals or barrier semaphores. Data moves between devices by JAX's collectives and lax.ppermute only.
A program may use at most 64 MiB of HBM per device.

```python
import jax
import jax.numpy as jnp
from jax import lax

D = 2048
KV_HEADS = 4
GROUP = 3
HEAD = 64
BLK = 32
TOPN = 16
CAP = 2
TOK_DEV = 256
HEADS = 12
SEQ = 8192
B = 4
KEY_BLOCKS = 256


def draw_tokens(key, part):
    base_key, scale_key = jax.random.split(key)
    return jnp.clip(jax.random.normal(base_key, (B, SEQ, D), jnp.float32), -6.0, 6.0).astype(jnp.bfloat16)


def draw_chosen(key, part):
    devices = SEQ // TOK_DEV
    blocks = TOK_DEV // BLK
    remote = blocks * (TOPN - 1)
    items = devices * CAP
    favour_key, pick_key, local_key, order_key = jax.random.split(key, 4)
    owner = jnp.arange(devices, dtype=jnp.int32)[None, None, :, None]
    device = jnp.arange(devices, dtype=jnp.int32)[None, :, None, None]
    copies = jnp.arange(CAP, dtype=jnp.int32)[None, None, None, :]
    shape = (B, devices, devices, CAP)
    favour = jax.random.randint(favour_key, (B, 1, devices, 1), 0, 4)
    taken = jax.random.randint(pick_key, shape, 0, 4) < favour
    forced = (owner == 0) | (copies == 0) & ((owner == device - 1) | (owner == device - devices // 2))
    level = jnp.where(owner < device, jnp.where(forced, 2, taken.astype(jnp.int32)), -1)
    item_index = owner * CAP + copies
    ranking = level * (items * items) + jax.random.randint(order_key, shape, 0, items) * items + item_index
    upper = jnp.broadcast_to((blocks - copies + CAP - 1) // CAP, shape)
    local_block = copies + CAP * jax.random.randint(local_key, shape, 0, upper)
    local_block = jnp.where((owner == 0) & (copies == 0), 0, local_block)
    global_id = jnp.where(level >= 1, owner * blocks + local_block, -1).reshape(B, devices, items)
    order = jnp.argsort(-ranking.reshape(B, devices, items), axis=-1)
    ranked = jnp.take_along_axis(global_id, order, axis=-1)
    if items >= remote:
        ranked = ranked[..., :remote]
    else:
        ranked = jnp.concatenate([ranked, jnp.full((B, devices, remote - items), -1, jnp.int32)], axis=-1)
    remote_part = jnp.swapaxes(ranked.reshape(B, devices, TOPN - 1, blocks), 2, 3)
    diagonal = jnp.arange(devices, dtype=jnp.int32)[:, None] * blocks + jnp.arange(blocks, dtype=jnp.int32)[None, :]
    diagonal = jnp.broadcast_to(diagonal[None, :, :, None], (B, devices, blocks, 1))
    listed = jnp.concatenate([diagonal, remote_part.astype(jnp.int32)], axis=-1)
    return listed.reshape(B, devices * blocks, TOPN).astype(jnp.int32)


def steps_of(rng, shape, shards, smallest, high):
    factor_of, own = 1.0, jax.random.fold_in(rng, 6)
    for axis_at, blocks in shards:
        draws = jnp.exp(jax.random.uniform(jax.random.fold_in(own, axis_at), (blocks,), jnp.float32, smallest / len(shards), high / len(shards)))
        factor_of = factor_of * jnp.repeat(draws, shape[axis_at] // blocks).reshape([-1 if axis == axis_at else 1 for axis in range(len(shape))])
    return factor_of


def noise(key, extent, deviation, reach, pieces=(), held_as=jnp.bfloat16):
    level = steps_of(key, extent, pieces, -0.22, 0.18) if pieces else 1.0
    drawn = jax.random.normal(key, extent, jnp.float32) * deviation * level
    return jnp.minimum(jnp.maximum(drawn, -reach), reach).astype(held_as)


def setup_inputs(seed: int = 0) -> dict:
    key_of = jax.random.split(jax.random.key(seed), 10)
    return {
        "tokens": draw_tokens(jax.random.fold_in(key_of[9], 71), 0),
        "query_weight": noise(key_of[1], (D, HEADS * HEAD), D ** -0.5, 0.125, ((1, 2),)),
        "key_weight": noise(key_of[2], (D, KV_HEADS * HEAD), D ** -0.5, 0.125, ((1, 2),)),
        "value_weight": noise(key_of[3], (D, KV_HEADS * HEAD), D ** -0.5, 0.125, ((1, 2),)),
        "gate_weight": noise(key_of[4], (D, 2 * HEADS), D ** -0.5, 0.125),
        "compress_weight": noise(key_of[5], (2, BLK, HEAD), BLK ** -0.5, 1.0, (), jnp.float32),
        "out_weight": noise(key_of[6], (HEADS * HEAD, D), (HEADS * HEAD) ** -0.5, 0.21875, ((0, 2),)),
        "out_gain": jnp.clip(1.0 + 0.18 * jax.random.normal(key_of[7], (D,), jnp.float32), 0.1, 1.9),
        "chosen": draw_chosen(jax.random.fold_in(key_of[9], 71), 0),
    }


neg_big = -1e+30
rope_base = 500000.0
norm_eps = 1e-06

def rotate(array_in, positions):
    half_dim = array_in.shape[-1] // 2
    inverse = rope_base ** (-jnp.arange(half_dim, dtype=jnp.float32) * (2.0 / array_in.shape[-1]))
    angles = positions.astype(jnp.float32)[:, None] * inverse[None, :]
    cosine = jnp.cos(angles)[:, None, :]
    sine_vals = jnp.sin(angles)[:, None, :]
    floats = array_in.astype(jnp.float32)
    first_half = floats[..., :half_dim]
    second_half = floats[..., half_dim:]
    turned = jnp.concatenate([first_half * cosine - second_half * sine_vals, second_half * cosine + first_half * sine_vals], axis=-1)
    return turned.astype(jnp.bfloat16)

def reference(tokens, query_weight, key_weight, value_weight, gate_weight, compress_weight, out_weight, out_gain, chosen):
    flattened = tokens.reshape(B * SEQ, D)
    queries = jnp.dot(flattened, query_weight, preferred_element_type=jnp.float32).astype(jnp.bfloat16)
    key_rows = jnp.dot(flattened, key_weight, preferred_element_type=jnp.float32).astype(jnp.bfloat16).reshape(B, SEQ, KV_HEADS, HEAD)
    values = jnp.dot(flattened, value_weight, preferred_element_type=jnp.float32).astype(jnp.bfloat16).reshape(B, SEQ, KV_HEADS, HEAD)
    gate_values = jax.nn.sigmoid(jnp.dot(flattened, gate_weight, preferred_element_type=jnp.float32)).reshape(B, SEQ, 2, KV_HEADS, GROUP)
    positions = jnp.arange(SEQ, dtype=jnp.int32)
    plain_query = queries.reshape(B, SEQ, KV_HEADS, GROUP, HEAD)
    turned_query = rotate(queries.reshape(B, SEQ, HEADS, HEAD), positions).reshape(B, SEQ, KV_HEADS, GROUP, HEAD)
    turned_keys = rotate(key_rows, positions)
    key_blocks = key_rows.reshape(B, KEY_BLOCKS, BLK, KV_HEADS, HEAD).astype(jnp.float32)
    val_blocks = values.reshape(B, KEY_BLOCKS, BLK, KV_HEADS, HEAD).astype(jnp.float32)
    packed_keys = jnp.einsum('bnjhd,jd->bnhd', key_blocks, compress_weight[0], precision=lax.Precision.HIGHEST).astype(jnp.bfloat16).astype(jnp.float32)
    packed_values = jnp.einsum('bnjhd,jd->bnhd', val_blocks, compress_weight[1], precision=lax.Precision.HIGHEST).astype(jnp.bfloat16).astype(jnp.float32)
    turned_blocks = turned_keys.reshape(B, KEY_BLOCKS, BLK, KV_HEADS, HEAD)
    value_blocks = values.reshape(B, KEY_BLOCKS, BLK, KV_HEADS, HEAD)
    score_scale = HEAD ** (-0.5)
    batch_index = jnp.arange(B, dtype=jnp.int32)[:, None]

    def one_block(block_index):
        first_row = block_index * BLK
        plain_block = lax.dynamic_slice_in_dim(plain_query, first_row, BLK, 1).astype(jnp.float32)
        turned_block = lax.dynamic_slice_in_dim(turned_query, first_row, BLK, 1).astype(jnp.float32)
        block_pos = first_row + jnp.arange(BLK, dtype=jnp.int32)
        scores = jnp.einsum('bqhgd,bnhd->bqhgn', plain_block, packed_keys) * score_scale
        visible = ((jnp.arange(KEY_BLOCKS, dtype=jnp.int32) + 1) * BLK - 1)[None, :] <= block_pos[:, None]
        keep_mask = visible[None, :, None, None, :]
        scores = jnp.where(keep_mask, scores, neg_big)
        peak = lax.optimization_barrier(jnp.max(scores, axis=-1, keepdims=True))
        powers = jnp.where(keep_mask, jnp.exp(scores - peak), 0.0)
        weight = (powers / jnp.maximum(lax.optimization_barrier(jnp.sum(powers, axis=-1, keepdims=True)), 1.0)).astype(jnp.bfloat16)
        weight = lax.optimization_barrier(weight).astype(jnp.float32)
        coarse_out = jnp.einsum('bqhgn,bnhd->bqhgd', weight, packed_values)
        picked = chosen[:, block_index]
        usable = picked >= 0
        clipped = jnp.maximum(picked, 0)
        sel_keys = turned_blocks[batch_index, clipped].astype(jnp.float32)
        sel_values = value_blocks[batch_index, clipped].astype(jnp.float32)
        key_pos = clipped[:, :, None] * BLK + jnp.arange(BLK, dtype=jnp.int32)[None, None, :]
        allowed = usable[:, None, :, None] & (key_pos[:, None, :, :] <= block_pos[None, :, None, None])
        fine_mask = allowed[:, :, None, None, :, :]
        fine = jnp.einsum('bqhgd,btjhd->bqhgtj', turned_block, sel_keys) * score_scale
        fine = jnp.where(fine_mask, fine, neg_big)
        fine_peak = lax.optimization_barrier(jnp.max(fine, axis=(-2, -1), keepdims=True))
        fine_powers = jnp.where(fine_mask, jnp.exp(fine - fine_peak), 0.0)
        fine_total = lax.optimization_barrier(jnp.sum(fine_powers, axis=(-2, -1)))
        rounded = lax.optimization_barrier(fine_powers.astype(jnp.bfloat16)).astype(jnp.float32)
        fine_out = jnp.einsum('bqhgtj,btjhd->bqhgd', rounded, sel_values) / fine_total[..., None]
        gate_block = lax.dynamic_slice_in_dim(gate_values, first_row, BLK, 1)
        mixed = gate_block[:, :, 0][..., None] * coarse_out + gate_block[:, :, 1][..., None] * fine_out
        return mixed.astype(jnp.bfloat16).reshape(B, BLK, HEADS * HEAD)
    hidden = lax.map(one_block, jnp.arange(KEY_BLOCKS, dtype=jnp.int32))
    hidden = jnp.moveaxis(hidden, 0, 1).reshape(B * SEQ, HEADS * HEAD)
    summed = jnp.dot(hidden, out_weight, preferred_element_type=jnp.float32)
    normed = summed * lax.rsqrt(lax.optimization_barrier(jnp.mean(summed * summed, axis=-1, keepdims=True)) + norm_eps) * out_gain
    return normed.astype(jnp.float32).reshape(B, SEQ, D)
```

```python
import functools

import jax
import jax.numpy as jnp
from jax import lax
from jax.experimental import pallas as pl
from jax.experimental.pallas import tpu as pltpu
from jax.sharding import PartitionSpec as P

HEAD = 64
BLK = 32
TOPN = 16
NEG = -1e30
ROPE_BASE = 500000.0
EPS = 1e-06
Z, Y = 8, 4
UNIT = 528
PIECE = 144
BF = jnp.bfloat16
F32 = jnp.float32


def dot(a, b):
    return jnp.dot(a, b, preferred_element_type=F32)


def dot_t(a, b):
    return lax.dot_general(a, b, (((1,), (1,)), ((), ())), preferred_element_type=F32)


def turn(x, cosine, sine):
    lane = lax.broadcasted_iota(jnp.int32, x.shape, 1)
    other = jnp.where(lane % HEAD < HEAD // 2, pltpu.roll(x, 96, 1), pltpu.roll(x, 32, 1))
    return x * cosine + other * sine


def kv_kernel(x_ref, wk_ref, wv_ref, cw_ref, cos_ref, sin_ref, out_ref):
    x = x_ref[...]
    keys = dot(x, wk_ref[...]).astype(BF).astype(F32)
    values = dot(x, wv_ref[...]).astype(BF)
    out_ref[pl.ds(0, 256), :] = turn(keys, cos_ref[...], sin_ref[...]).astype(BF)
    out_ref[pl.ds(256, 256), :] = values

    def compress(rows, weight):
        wide = jnp.concatenate([weight, weight], axis=1)
        return jnp.sum(rows.reshape(8, BLK, 128) * wide[None], axis=1)

    packed = jnp.concatenate(
        [compress(keys, cw_ref[0]), compress(values.astype(F32), cw_ref[1])], axis=0
    )
    out_ref[pl.ds(512, 16), :] = packed.astype(BF)


def q_kernel(x_ref, wq_ref, wg_ref, cos_ref, sin_ref, plain_ref, turned_ref, gate_ref):
    x = x_ref[...]
    gate_ref[...] = jax.nn.sigmoid(dot(x, wg_ref[...]))
    lane = lax.broadcasted_iota(jnp.int32, (256, 128), 1)
    for pair in range(3):
        q = dot(x, wq_ref[:, pl.ds(pair * 128, 128)]).astype(BF).astype(F32)
        t = turn(q, cos_ref[...], sin_ref[...]).astype(BF).astype(F32)
        for half in range(2):
            head = pair * 2 + half
            side = head // 3
            keep = (lane >= HEAD) if side else (lane < HEAD)
            for src, dst in ((q, plain_ref), (t, turned_ref)):
                rows = src if half == side else pltpu.roll(src, 64, 1)
                rows = jnp.where(keep, rows * 0.125, 0.0).astype(BF)
                for i in range(8):
                    dst[i, pl.ds(head * BLK, BLK), :] = rows[i * BLK : (i + 1) * BLK]


def select_kernel(low_ref, high_ref, *refs):
    units, outs = refs[:Z], refs[Z:]
    for d in range(3):
        for r in range(Z):
            unit, out = units[r], outs[d]
            for slot, table in ((0, low_ref), (1, high_ref)):
                row = pl.multiple_of(table[d, r] * BLK, BLK)
                out[pl.ds(r * PIECE + slot * BLK, BLK), :] = unit[pl.ds(row, BLK), :]
                out[pl.ds(r * PIECE + 64 + slot * BLK, BLK), :] = unit[pl.ds(row + 256, BLK), :]
            out[pl.ds(r * PIECE + 128, 16), :] = unit[pl.ds(512, 16), :]


def attend_kernel(where_ref, krow_ref, vrow_ref, bias_ref, plain_ref, turned_ref, gate_ref, *refs):
    units, pieces = refs[:Z], refs[Z : Z + 3]
    keep_ref, send_ref, pool, sk, sv, kg, vg = refs[Z + 3 :]
    z, y, core = where_ref[0], where_ref[1], where_ref[2]
    for r in range(Z):
        pool[pl.ds(r * UNIT, 512), :] = units[r][pl.ds(0, 512), :]
        sk[pl.ds(r * 8, 8), :] = units[r][pl.ds(512, 8), :]
        sv[pl.ds(r * 8, 8), :] = units[r][pl.ds(520, 8), :]
        for d in range(3):
            base = Z * UNIT + d * Z * PIECE + r * PIECE
            pool[pl.ds(base, 128), :] = pieces[d][pl.ds(r * PIECE, 128), :]
            sk[pl.ds((d + 1) * 64 + r * 8, 8), :] = pieces[d][pl.ds(r * PIECE + 128, 8), :]
            sv[pl.ds((d + 1) * 64 + r * 8, 8), :] = pieces[d][pl.ds(r * PIECE + 136, 8), :]

    column = lax.broadcasted_iota(jnp.int32, (192, 256), 1)
    row = lax.broadcasted_iota(jnp.int32, (192, 256), 0) % BLK
    dev = ((z - (column // 8) % 8 + 8) % 8) * Y + (y - column // 64 + Y) % Y
    block_id = dev * 8 + column % 8
    own_first = (z * Y + y) * 8
    triangle = jnp.where(
        (column[:, :128] < BLK) & (column[:, :128] > row[:, :128]), NEG, 0.0
    )
    lane = lax.broadcasted_iota(jnp.int32, (BLK, 128), 1)
    coarse_keys, coarse_values = sk[...], sv[...]

    for step in range(8):
        i = lax.rem(step + 4 * (1 - core), 8)
        for t in range(TOPN):
            krow = pl.multiple_of(krow_ref[i, t], 16)
            vrow = pl.multiple_of(vrow_ref[i, t], 16)
            kg[step % 2, pl.ds(t * BLK, BLK), :] = pool[pl.ds(krow, BLK), :]
            vg[step % 2, pl.ds(t * BLK, BLK), :] = pool[pl.ds(vrow, BLK), :]
        scores = dot_t(plain_ref[i], coarse_keys)
        own = own_first + i
        visible = (block_id < own) | ((block_id == own) & (row == BLK - 1))
        scores = jnp.where(visible, scores, NEG)
        peak = jnp.max(scores, axis=-1, keepdims=True)
        powers = jnp.where(visible, jnp.exp(scores - peak), 0.0)
        total = jnp.maximum(jnp.sum(powers, axis=-1, keepdims=True), 1.0)
        weight = (powers * (1.0 / total)).astype(BF)
        coarse = dot(weight, coarse_values)

        fine = dot_t(turned_ref[i], kg[step % 2]) + bias_ref[pl.ds(i, 1), :]
        fine = jnp.concatenate([fine[:, :128] + triangle, fine[:, 128:]], axis=1)
        fine_peak = jnp.max(fine, axis=-1, keepdims=True)
        fine_powers = jnp.exp(fine - fine_peak)
        fine_total = jnp.sum(fine_powers, axis=-1, keepdims=True)
        fine_out = dot(fine_powers.astype(BF), vg[step % 2]) * (1.0 / fine_total)

        gates = gate_ref[pl.ds(pl.multiple_of(i * BLK, BLK), BLK), :]
        heads = []
        for head in range(6):
            pick = []
            for base in (0, 12):
                low = gates[:, base + head : base + head + 1]
                high = gates[:, base + 6 + head : base + 7 + head]
                pick.append(jnp.where(core == 0, low, high))
            span = slice(head * BLK, (head + 1) * BLK)
            heads.append(pick[0] * coarse[span] + pick[1] * fine_out[span])
        groups = (
            jnp.where(lane < HEAD, heads[0], pltpu.roll(heads[1], 64, 1)),
            jnp.where(lane < HEAD, heads[2], heads[3]),
            jnp.where(lane < HEAD, pltpu.roll(heads[4], 64, 1), heads[5]),
        )
        target = send_ref if step < 4 else keep_ref
        for g in range(3):
            target[pl.ds((step % 4) * BLK, BLK), pl.ds(g * 128, 128)] = groups[g].astype(BF)


def out_kernel(keep_ref, got_ref, w_own_ref, w_other_ref, gain_ref, out_ref):
    summed = dot(keep_ref[...], w_own_ref[...]) + dot(got_ref[...], w_other_ref[...])
    mean = jnp.mean(summed * summed, axis=-1, keepdims=True)
    out_ref[...] = summed * lax.rsqrt(mean + EPS) * gain_ref[...]


VMEM = pl.BlockSpec(memory_space=pltpu.VMEM)
SMEM = pl.BlockSpec(memory_space=pltpu.SMEM)


def call(kernel, name, out_shape, specs, args, scratch=(), flops=0, data=0):
    return pl.pallas_call(
        kernel,
        name=name,
        out_shape=out_shape,
        in_specs=specs,
        out_specs=jax.tree.map(lambda _: VMEM, out_shape),
        scratch_shapes=scratch,
        compiler_params=pltpu.CompilerParams(vmem_limit_bytes=40 * 2**20),
        cost_estimate=pl.CostEstimate(flops=flops, bytes_accessed=data, transcendentals=0),
    )(*args)


def z_shift(d):
    return [(z * Y + y, (z + d) % Z * Y + y) for z in range(Z) for y in range(Y)]


def y_shift(d):
    return [(z * Y + y, z * Y + (y + d) % Y) for z in range(Z) for y in range(Y)]


def rope_tables(positions):
    half = HEAD // 2
    inverse = ROPE_BASE ** (-jnp.arange(half, dtype=F32) * (2.0 / HEAD))
    angles = positions.astype(F32)[:, None] * inverse[None, :]
    cosine, sine = jnp.cos(angles), jnp.sin(angles)
    return (
        jnp.concatenate([cosine] * 4, axis=-1),
        jnp.concatenate([-sine, sine, -sine, sine], axis=-1),
    )


def on_device(
    tokens,
    query_weight,
    key_weight,
    value_weight,
    gate_weight,
    compress_weight,
    out_weight,
    out_gain,
    chosen,
):
    shape = jax.ShapeDtypeStruct
    x = tokens[0]
    index = lax.axis_index("kv")
    z, y = index // Y, index % Y
    core = lax.axis_index("tp")
    listed = chosen[0]
    asked = [lax.ppermute(listed, "kv", y_shift(-d)) for d in (1, 2, 3)]
    other_weight = lax.ppermute(out_weight, "tp", [(0, 1), (1, 0)])

    cosine, sine = rope_tables(index * 256 + jnp.arange(256, dtype=jnp.int32))
    unit = call(
        kv_kernel,
        "kv",
        shape((UNIT, 128), BF),
        [VMEM] * 6,
        (x, key_weight, value_weight, compress_weight, cosine, sine),
        flops=2 * 256 * 2048 * 256,
        data=2 * 2**20,
    )
    far = {0: unit}
    for d in (1, 7, 2, 6, 3, 5, 4):
        far[d] = lax.ppermute(unit, "kv", z_shift(d))
    units = [far[r] for r in range(Z)]

    plain, turned, gates = call(
        q_kernel,
        "q",
        (shape((8, 192, 128), BF), shape((8, 192, 128), BF), shape((256, 24), F32)),
        [VMEM] * 5,
        (x, query_weight, gate_weight, cosine, sine),
        flops=2 * 256 * 2048 * 408,
        data=3 * 2**20,
    )

    asked = jnp.stack(asked).reshape(3, 1, 8 * TOPN)
    sources = (z - jnp.arange(Z, dtype=jnp.int32)) % Z * Y + y
    hit = (asked >> 3) == sources[None, :, None]
    low = jnp.min(jnp.where(hit, asked & 7, 7), axis=-1)
    high = jnp.max(jnp.where(hit, asked & 7, 0), axis=-1)
    pieces = call(
        select_kernel,
        "select",
        (shape((Z * PIECE, 128), BF),) * 3,
        [SMEM, SMEM] + [VMEM] * Z,
        (low, high, *units),
        flops=2**20,
        data=2 * 2**20,
    )
    pieces = [lax.ppermute(p, "kv", y_shift(d)) for p, d in zip(pieces, (1, 2, 3))]

    flat = listed.reshape(-1)
    owner = flat >> 3
    second = jnp.any(
        (owner[:, None] == owner[None, :]) & (flat[None, :] < flat[:, None]), axis=1
    ).astype(jnp.int32)
    block = jnp.maximum(flat, 0)
    owner = block >> 3
    r = (z - owner // Y) % Z
    d = (y - owner % Y) % Y
    mine = d == 0
    base = jnp.where(
        mine, r * UNIT + (block & 7) * BLK, Z * UNIT + (d - 1) * Z * PIECE + r * PIECE + second * BLK
    )
    krow = base.reshape(8, TOPN)
    vrow = (base + jnp.where(mine, 256, 64)).reshape(8, TOPN)
    bias = jnp.repeat(jnp.where(listed >= 0, 0.0, NEG).astype(F32), BLK, axis=1)

    keep, send = call(
        attend_kernel,
        "attend",
        (shape((128, 384), BF), shape((128, 384), BF)),
        [SMEM] * 3 + [VMEM] * (4 + Z + 3),
        (jnp.stack([z, y, core]), krow, vrow, bias, plain, turned, gates, *units, *pieces),
        scratch=[
            pltpu.VMEM((Z * UNIT + 3 * Z * PIECE, 128), BF),
            pltpu.VMEM((256, 128), BF),
            pltpu.VMEM((256, 128), BF),
            pltpu.VMEM((2, 512, 128), BF),
            pltpu.VMEM((2, 512, 128), BF),
        ],
        flops=2**30,
        data=4 * 2**20,
    )
    got = lax.ppermute(send, "tp", [(0, 1), (1, 0)])
    out = call(
        out_kernel,
        "project",
        shape((128, 2048), F32),
        [VMEM] * 5,
        (keep, got, out_weight, other_weight, out_gain[None]),
        flops=2 * 128 * 768 * 2048,
        data=4 * 2**20,
    )
    return out[None]


def solution(mesh):
    in_specs = (
        P("dp", "kv", None),
        P(None, "tp"),
        P(None, "tp"),
        P(None, "tp"),
        P(),
        P(),
        P("tp", None),
        P(),
        P("dp", "kv", None),
    )
    out_specs = P("dp", ("kv", "tp"), None)
    return jax.shard_map(
        on_device, mesh=mesh, in_specs=in_specs, out_specs=out_specs, check_vma=False
    )
```

```python
import jax
import jax.numpy as jnp
from jax import lax
from jax.experimental import pallas as pl
from jax.experimental.pallas import tpu as pltpu
from jax.sharding import PartitionSpec as P


HEAD = 64
BLK = 32
TOPN = 16
NEG = -1e30
ROPE_BASE = 500000.0
EPS = 1e-06
Z, Y = 8, 4
UNIT = 528
SHARE = 576
PIECE = 144
BF = jnp.bfloat16
F32 = jnp.float32


def dot(a, b):
    return jnp.dot(a, b, preferred_element_type=F32)


def dot_t(a, b):
    return lax.dot_general(a, b, (((1,), (1,)), ((), ())), preferred_element_type=F32)


def turn(x, cosine, sine):
    lane = lax.broadcasted_iota(jnp.int32, x.shape, 1)
    other = jnp.where(lane % HEAD < HEAD // 2, pltpu.roll(x, 96, 1), pltpu.roll(x, 32, 1))
    return x * cosine + other * sine


def kv_kernel(after_ref, x_ref, wk_ref, wv_ref, cw_ref, cos_ref, sin_ref, out_ref):
    x = x_ref[...]
    keys = dot(x, wk_ref[...]).astype(BF).astype(F32)
    out_ref[pl.ds(0, 256), :] = turn(keys, cos_ref[...], sin_ref[...]).astype(BF)
    values = dot(x, wv_ref[...]).astype(BF)
    out_ref[pl.ds(256, 256), :] = values

    def compress(rows, weight):
        wide = jnp.concatenate([weight, weight], axis=1)
        return jnp.sum(rows.reshape(8, BLK, 128) * wide[None], axis=1)

    packed = jnp.concatenate(
        [compress(keys, cw_ref[0]), compress(values.astype(F32), cw_ref[1])], axis=0
    )
    out_ref[pl.ds(512, 16), :] = packed.astype(BF)


def table_kernel(scalar_ref, listed_ref, ask_ref, rows_ref, bias_ref):
    z = lax.axis_index("kv") // Y
    listed = listed_ref[...]
    lane = lax.broadcasted_iota(jnp.int32, (8, 128), 1)
    low, high = jnp.full((8, 128), 7, jnp.int32), jnp.zeros((8, 128), jnp.int32)
    for g in range(4):
        row = jnp.zeros((8, 128), F32)
        for part in range(4):
            entry = jnp.broadcast_to(listed[:, g * 4 + part : g * 4 + part + 1], (8, 128))
            hit = (entry >> 3) == lane
            low = jnp.minimum(low, jnp.where(hit, entry & 7, 7))
            high = jnp.maximum(high, jnp.where(hit, entry & 7, 0))
            row = jnp.where((lane >> 5) == part, jnp.where(entry >= 0, 0.0, NEG), row)
        bias_ref[:, pl.ds(g * 128, 128)] = row
    low = jnp.min(low, axis=0, keepdims=True)
    high = jnp.max(high, axis=0, keepdims=True)
    first = lax.broadcasted_iota(jnp.int32, (8, 128), 0) == 0
    ask_ref[...] = jnp.where(first, low, high)
    owner = listed >> 3
    second = jnp.zeros((8, TOPN), jnp.int32)
    for i in range(8):
        for t in range(TOPN):
            other = scalar_ref[i, t]
            second = jnp.where((owner == (other >> 3)) & (other < listed), 1, second)
    owner = jnp.maximum(listed, 0) >> 3
    owner_z = owner >> 2
    sender = (z // 2) * 2 + (owner_z & 1)
    u = ((sender - owner_z) & 7) >> 1
    rows_ref[...] = ((owner_z & 1) * Y + (owner & 3)) * SHARE + u * PIECE + second * BLK


def q_kernel(
    x_ref, wq_ref, wg_hbm, cos_ref, sin_ref, plain_ref, turned_ref, gate_ref, wg_ref, sem
):
    copy = pltpu.make_async_copy(wg_hbm, wg_ref, sem)
    copy.start()
    x = x_ref[...]
    lane = lax.broadcasted_iota(jnp.int32, (256, 128), 1)
    for pair in range(3):
        q = dot(x, wq_ref[:, pl.ds(pair * 128, 128)]).astype(BF).astype(F32)
        t = turn(q, cos_ref[...], sin_ref[...]).astype(BF).astype(F32)
        for half in range(2):
            head = pair * 2 + half
            side = head // 3
            keep = (lane >= HEAD) if side else (lane < HEAD)
            for src, dst in ((q, plain_ref), (t, turned_ref)):
                rows = src if half == side else pltpu.roll(src, 64, 1)
                rows = jnp.where(keep, rows * 0.125, 0.0).astype(BF)
                for i in range(8):
                    dst[i, pl.ds(head * BLK, BLK), :] = rows[i * BLK : (i + 1) * BLK]
    copy.wait()
    gate_ref[...] = jax.nn.sigmoid(dot(x, wg_ref[...]))


def select_kernel(*refs):
    asks, units, out = refs[:Y], refs[Y : Y + 4], refs[Y + 4]
    index = lax.axis_index("kv")
    z, y = index // Y, index % Y
    for d in range(Y):
        for partner in range(2):
            dest = lax.rem(z + partner, 2) * Y + lax.rem(y + d, Y)
            for u in range(4):
                base = pl.multiple_of(dest * SHARE + u * PIECE, 16)
                source = lax.rem(z - 2 * u + Z, Z) * Y + y
                for slot in range(2):
                    row = pl.multiple_of(asks[d][partner * 8 + slot, source] * BLK, BLK)
                    out[pl.ds(base + slot * BLK, BLK), :] = units[u][pl.ds(row, BLK), :]
                    out[pl.ds(base + 64 + slot * BLK, BLK), :] = units[u][pl.ds(row + 256, BLK), :]
                out[pl.ds(base + 128, 16), :] = units[u][pl.ds(512, 16), :]


def attend_kernel(
    row_ref, bias_ref, plain_ref, turned_ref, gate_ref, unit_ref, pool, *refs
):
    keep_ref, send_ref, sk, sv, kg, vg = refs
    index = lax.axis_index("kv")
    z, y, core = index // Y, index % Y, lax.axis_index("tp")
    for piece in range(32):
        base = piece * PIECE + 128
        sk[pl.ds(piece * 8, 8), :] = pool[pl.ds(base, 8), :]
        sv[pl.ds(piece * 8, 8), :] = pool[pl.ds(base + 8, 8), :]

    column = lax.broadcasted_iota(jnp.int32, (192, 256), 1)
    row = lax.broadcasted_iota(jnp.int32, (192, 256), 0) % BLK
    sender = (z // 2) * 2 + column // 128
    dev = ((sender - 2 * (column // 8 % 4) + Z) % Z) * Y + column // 32 % Y
    block_id = dev * 8 + column % 8
    own_first = (z * Y + y) * 8
    triangle = jnp.where(
        (column[:, :128] < BLK) & (column[:, :128] > row[:, :128]), NEG, 0.0
    )
    lane = lax.broadcasted_iota(jnp.int32, (BLK, 128), 1)
    coarse_keys, coarse_values = sk[...], sv[...]

    for step in range(8):
        i = lax.rem(step + 4 * (1 - core), 8)
        own_row = pl.multiple_of(i * BLK, BLK)
        kg[step % 2, pl.ds(0, BLK), :] = unit_ref[pl.ds(own_row, BLK), :]
        vg[step % 2, pl.ds(0, BLK), :] = unit_ref[pl.ds(own_row + 256, BLK), :]
        for t in range(1, TOPN):
            at = pl.multiple_of(row_ref[i, t], 16)
            kg[step % 2, pl.ds(t * BLK, BLK), :] = pool[pl.ds(at, BLK), :]
            vg[step % 2, pl.ds(t * BLK, BLK), :] = pool[pl.ds(at + 64, BLK), :]
        scores = dot_t(plain_ref[i], coarse_keys)
        own = own_first + i
        visible = (block_id < own) | ((block_id == own) & (row == BLK - 1))
        scores = jnp.where(visible, scores, NEG)
        peak = jnp.max(scores, axis=-1, keepdims=True)
        powers = jnp.where(visible, jnp.exp(scores - peak), 0.0)
        total = jnp.maximum(jnp.sum(powers, axis=-1, keepdims=True), 1.0)
        weight = (powers * (1.0 / total)).astype(BF)
        coarse = dot(weight, coarse_values)

        fine = dot_t(turned_ref[i], kg[step % 2]) + bias_ref[pl.ds(i, 1), :]
        fine = jnp.concatenate([fine[:, :128] + triangle, fine[:, 128:]], axis=1)
        fine_peak = jnp.max(fine, axis=-1, keepdims=True)
        fine_powers = jnp.exp(fine - fine_peak)
        fine_total = jnp.sum(fine_powers, axis=-1, keepdims=True)
        fine_out = dot(fine_powers.astype(BF), vg[step % 2]) * (1.0 / fine_total)

        gates = gate_ref[pl.ds(pl.multiple_of(i * BLK, BLK), BLK), :]
        heads = []
        for head in range(6):
            pick = []
            for base in (0, 12):
                low = gates[:, base + head : base + head + 1]
                high = gates[:, base + 6 + head : base + 7 + head]
                pick.append(jnp.where(core == 0, low, high))
            span = slice(head * BLK, (head + 1) * BLK)
            heads.append(pick[0] * coarse[span] + pick[1] * fine_out[span])
        groups = (
            jnp.where(lane < HEAD, heads[0], pltpu.roll(heads[1], 64, 1)),
            jnp.where(lane < HEAD, heads[2], heads[3]),
            jnp.where(lane < HEAD, pltpu.roll(heads[4], 64, 1), heads[5]),
        )
        target = send_ref if step < 4 else keep_ref
        for g in range(3):
            target[pl.ds((step % 4) * BLK, BLK), pl.ds(g * 128, 128)] = groups[g].astype(BF)


def out_kernel(keep_ref, got_ref, w_own_ref, w_other_ref, gain_ref, out_ref):
    summed = dot(keep_ref[...], w_own_ref[...]) + dot(got_ref[...], w_other_ref[...])
    mean = jnp.mean(summed * summed, axis=-1, keepdims=True)
    out_ref[...] = summed * lax.rsqrt(mean + EPS) * gain_ref[...]


VMEM = pl.BlockSpec(memory_space=pltpu.VMEM)
HBM = pl.BlockSpec(memory_space=pltpu.HBM)
SMEM = pl.BlockSpec(memory_space=pltpu.SMEM)


def call(kernel, out_shape, specs, args, scratch=(), flops=0, data=0, vmem=12 * 2**20):
    return pl.pallas_call(
        kernel,
        out_shape=out_shape,
        in_specs=specs,
        out_specs=jax.tree.map(lambda _: VMEM, out_shape),
        scratch_shapes=scratch,
        compiler_params=pltpu.CompilerParams(vmem_limit_bytes=vmem),
        cost_estimate=pl.CostEstimate(flops=flops, bytes_accessed=data, transcendentals=0),
    )(*args)


def z_shift(d):
    return [(z * Y + y, (z + d) % Z * Y + y) for z in range(Z) for y in range(Y)]


def y_shift(d):
    return [(z * Y + y, z * Y + (y + d) % Y) for z in range(Z) for y in range(Y)]


def z_pair():
    return [(z * Y + y, (z ^ 1) * Y + y) for z in range(Z) for y in range(Y)]


def pair_groups():
    return [[(2 * p + a) * Y + y for a in range(2) for y in range(Y)] for p in range(Z // 2)]


def rope_tables(positions):
    half = HEAD // 2
    inverse = ROPE_BASE ** (-jnp.arange(half, dtype=F32) * (2.0 / HEAD))
    angles = positions.astype(F32)[:, None] * inverse[None, :]
    cosine, sine = jnp.cos(angles), jnp.sin(angles)
    return (
        jnp.concatenate([cosine] * 4, axis=-1),
        jnp.concatenate([-sine, sine, -sine, sine], axis=-1),
    )


def on_device(
    tokens,
    query_weight,
    key_weight,
    value_weight,
    gate_weight,
    compress_weight,
    out_weight,
    out_gain,
    chosen,
):
    shape = jax.ShapeDtypeStruct
    x = tokens[0]
    index = lax.axis_index("kv")
    other_weight = lax.ppermute(out_weight, "tp", [(0, 1), (1, 0)])
    ask, rows, bias = call(
        table_kernel,
        (
            shape((8, 128), jnp.int32),
            shape((8, TOPN), jnp.int32),
            shape((8, TOPN * BLK), F32),
        ),
        [SMEM, VMEM],
        (chosen[0], chosen[0]),
        flops=2**32,
        data=2**12,
    )
    partner_ask = lax.ppermute(ask, "kv", z_pair())

    cosine, sine = rope_tables(index * 256 + jnp.arange(256, dtype=jnp.int32))
    unit = call(
        kv_kernel,
        shape((UNIT, 128), BF),
        [VMEM] * 7,
        (ask, x, key_weight, value_weight, compress_weight, cosine, sine),
        flops=2 * 256 * 2048 * 256,
        data=2 * 2**20,
    )
    units = [unit] + [lax.ppermute(unit, "kv", z_shift(d)) for d in (2, 4, 6)]
    asks = jnp.concatenate([ask, partner_ask])
    asks = [asks] + [lax.ppermute(asks, "kv", y_shift(-d)) for d in (1, 2, 3)]

    plain, turned, gates = call(
        q_kernel,
        (shape((8, 192, 128), BF), shape((8, 192, 128), BF), shape((256, 24), F32)),
        [VMEM, VMEM, HBM, VMEM, VMEM],
        (x, query_weight, gate_weight, cosine, sine),
        scratch=[pltpu.VMEM(gate_weight.shape, BF), pltpu.SemaphoreType.DMA],
        flops=2 * 256 * 2048 * 408,
        data=3 * 2**20,
    )
    share = call(
        select_kernel,
        shape((8 * SHARE, 128), BF),
        [SMEM] * 4 + [VMEM] * 4,
        (*asks, *units),
        flops=2**20,
        data=2 * 2**20,
    )
    pool = lax.all_to_all(
        share.reshape(8, SHARE, 128), "kv", 0, 0, tiled=True, axis_index_groups=pair_groups()
    ).reshape(8 * SHARE, 128)

    keep, send = call(
        attend_kernel,
        (shape((128, 384), BF), shape((128, 384), BF)),
        [SMEM] + [VMEM] * 6,
        (rows, bias, plain, turned, gates, unit, pool),
        scratch=[
            pltpu.VMEM((256, 128), BF),
            pltpu.VMEM((256, 128), BF),
            pltpu.VMEM((2, 512, 128), BF),
            pltpu.VMEM((2, 512, 128), BF),
        ],
        flops=2**30,
        data=4 * 2**20,
        vmem=58720256,
    )
    got = lax.ppermute(send, "tp", [(0, 1), (1, 0)])
    out = call(
        out_kernel,
        shape((128, 2048), F32),
        [VMEM] * 5,
        (keep, got, out_weight, other_weight, out_gain[None]),
        flops=2 * 128 * 768 * 2048,
        data=4 * 2**20,
    )
    return out[None]


def solution(mesh):
    in_specs = (
        P("dp", "kv", None),
        P(None, "tp"),
        P(None, "tp"),
        P(None, "tp"),
        P(),
        P(),
        P("tp", None),
        P(),
        P("dp", "kv", None),
    )
    out_specs = P("dp", ("kv", "tp"), None)

    return jax.shard_map(
        on_device, mesh=mesh, in_specs=in_specs, out_specs=out_specs, check_vma=False
    )
```

```python
import jax
import jax.numpy as jnp
from jax import lax
from jax.experimental import pallas as pl
from jax.experimental.pallas import tpu as pltpu
from jax.sharding import PartitionSpec as P


HEAD = 64
BLK = 32
TOPN = 16
NEG = -1e30
ROPE_BASE = 500000.0
EPS = 1e-06
Z, Y = 8, 4
UNIT = 528
SHARE = 576
PIECE = 144
BF = jnp.bfloat16
F32 = jnp.float32


def dot(a, b):
    return jnp.dot(a, b, preferred_element_type=F32)


def dot_t(a, b):
    return lax.dot_general(a, b, (((1,), (1,)), ((), ())), preferred_element_type=F32)


def turn(x, cosine, sine):
    lane = lax.broadcasted_iota(jnp.int32, x.shape, 1)
    other = jnp.where(lane % HEAD < HEAD // 2, pltpu.roll(x, 96, 1), pltpu.roll(x, 32, 1))
    return x * cosine + other * sine


def kv_kernel(after_ref, x_ref, wk_ref, wv_ref, cw_ref, cos_ref, sin_ref, out_ref):
    x = x_ref[...]
    keys = dot(x, wk_ref[...]).astype(BF).astype(F32)
    out_ref[pl.ds(0, 256), :] = turn(keys, cos_ref[...], sin_ref[...]).astype(BF)
    values = dot(x, wv_ref[...]).astype(BF)
    out_ref[pl.ds(256, 256), :] = values

    def compress(rows, weight):
        wide = jnp.concatenate([weight, weight], axis=1)
        return jnp.sum(rows.reshape(8, BLK, 128) * wide[None], axis=1)

    packed = jnp.concatenate(
        [compress(keys, cw_ref[0]), compress(values.astype(F32), cw_ref[1])], axis=0
    )
    out_ref[pl.ds(512, 16), :] = packed.astype(BF)


def ask_kernel(listed_ref, ask_ref):
    listed = listed_ref[...]
    lane = lax.broadcasted_iota(jnp.int32, (8, 128), 1)
    low, high = jnp.full((8, 128), 7, jnp.int32), jnp.zeros((8, 128), jnp.int32)
    for t in range(TOPN):
        entry = jnp.broadcast_to(listed[:, t : t + 1], (8, 128))
        hit = (entry >> 3) == lane
        low = jnp.minimum(low, jnp.where(hit, entry & 7, 7))
        high = jnp.maximum(high, jnp.where(hit, entry & 7, 0))
    low = jnp.min(low, axis=0, keepdims=True)
    high = jnp.max(high, axis=0, keepdims=True)
    first = lax.broadcasted_iota(jnp.int32, (8, 128), 0) == 0
    ask_ref[...] = jnp.where(first, low, high)


def fill_tables(scalar_ref, listed, rows_ref, bias_ref):
    z = lax.axis_index("kv") // Y
    lane = lax.broadcasted_iota(jnp.int32, (8, 128), 1)
    for g in range(4):
        row = jnp.zeros((8, 128), F32)
        for part in range(4):
            entry = jnp.broadcast_to(listed[:, g * 4 + part : g * 4 + part + 1], (8, 128))
            row = jnp.where((lane >> 5) == part, jnp.where(entry >= 0, 0.0, NEG), row)
        bias_ref[:, pl.ds(g * 128, 128)] = row
    owner = listed >> 3
    second = jnp.zeros((8, TOPN), jnp.int32)
    for i in range(8):
        for t in range(TOPN):
            other = scalar_ref[i, t]
            second = jnp.where((owner == (other >> 3)) & (other < listed), 1, second)
    owner = jnp.maximum(listed, 0) >> 3
    owner_z = owner >> 2
    sender = (z // 2) * 2 + (owner_z & 1)
    u = ((sender - owner_z) & 7) >> 1
    rows_ref[...] = ((owner_z & 1) * Y + (owner & 3)) * SHARE + u * PIECE + second * BLK


def q_kernel(scalar_ref, listed_ref, x_ref, wq_ref, wg_ref, cos_ref, sin_ref, *outs):
    plain_ref, turned_ref, gate_ref, rows_ref, bias_ref = outs
    fill_tables(scalar_ref, listed_ref[...], rows_ref, bias_ref)
    x = x_ref[...]
    logits = dot_t(wg_ref[...], x)
    first_core = lax.axis_index("tp") == 0
    for branch in range(2):
        at = branch * 12
        own = jnp.where(first_core, logits[at : at + 6], logits[at + 6 : at + 12])
        gate_ref[branch * 8 : branch * 8 + 6, :] = jax.nn.sigmoid(own)
    lane = lax.broadcasted_iota(jnp.int32, (256, 128), 1)
    plain, turned = [], []
    for pair in range(3):
        q = dot(x, wq_ref[:, pl.ds(pair * 128, 128)]).astype(BF).astype(F32)
        plain.append(q * 0.125)
        turned.append(turn(q, cos_ref[...], sin_ref[...]).astype(BF).astype(F32) * 0.125)
    for tiles, out in ((plain, plain_ref), (turned, turned_ref)):
        groups = (
            jnp.where(lane < HEAD, tiles[0], tiles[1]),
            jnp.where(lane < HEAD, pltpu.roll(tiles[0], 64, 1), pltpu.roll(tiles[2], 64, 1)),
            jnp.where(lane < HEAD, tiles[1], tiles[2]),
        )
        for g in range(3):
            out[:, pl.ds(g * 128, 128)] = groups[g].astype(BF)


def select_kernel(*refs):
    asks, units, out = refs[:Y], refs[Y : Y + 4], refs[Y + 4]
    index = lax.axis_index("kv")
    z, y = index // Y, index % Y
    for d in range(Y):
        for partner in range(2):
            dest = lax.rem(z + partner, 2) * Y + lax.rem(y + d, Y)
            for u in range(4):
                base = pl.multiple_of(dest * SHARE + u * PIECE, 16)
                source = lax.rem(z - 2 * u + Z, Z) * Y + y
                for slot in range(2):
                    row = pl.multiple_of(asks[d][partner * 8 + slot, source] * BLK, BLK)
                    out[pl.ds(base + slot * BLK, BLK), :] = units[u][pl.ds(row, BLK), :]
                    out[pl.ds(base + 64 + slot * BLK, BLK), :] = units[u][pl.ds(row + 256, BLK), :]
                out[pl.ds(base + 128, 16), :] = units[u][pl.ds(512, 16), :]


def attend_kernel(
    row_ref, bias_ref, plain_ref, turned_ref, gate_ref, unit_ref, pool, *refs
):
    keep_ref, send_ref, sk, sv, kg, vg, limit_ref, flip_ref = refs
    index = lax.axis_index("kv")
    z, core = index // Y, lax.axis_index("tp")
    blocks = [lax.rem(step + 4 * (1 - core), 8) for step in range(8)]
    starts = [pl.multiple_of(i * BLK, BLK) for i in blocks]
    for piece in range(32):
        base = piece * PIECE + 128
        sk[pl.ds(piece * 8, 8), :] = pool[pl.ds(base, 8), :]
        sv[pl.ds(piece * 8, 8), :] = pool[pl.ds(base + 8, 8), :]
    for step in range(8):
        kg[step, pl.ds(0, BLK), :] = unit_ref[pl.ds(starts[step], BLK), :]
        vg[step, pl.ds(0, BLK), :] = unit_ref[pl.ds(starts[step] + 256, BLK), :]
        for t in range(1, TOPN):
            at = pl.multiple_of(row_ref[blocks[step], t], 16)
            kg[step, pl.ds(t * BLK, BLK), :] = pool[pl.ds(at, BLK), :]
            vg[step, pl.ds(t * BLK, BLK), :] = pool[pl.ds(at + 64, BLK), :]

    column = lax.broadcasted_iota(jnp.int32, (192, 256), 1)
    row = lax.broadcasted_iota(jnp.int32, (192, 256), 0) % BLK
    sender = (z // 2) * 2 + column // 128
    dev = ((sender - 2 * (column // 8 % 4) + Z) % Z) * Y + column // 32 % Y
    limit_ref[...] = (dev * 8 + column % 8) * BLK + (BLK - 1) - row
    triangle = jnp.where(
        (column[:, :128] < BLK) & (column[:, :128] > row[:, :128]), NEG, 0.0
    )
    lane = lax.broadcasted_iota(jnp.int32, (BLK, 128), 1)
    low = lane < HEAD
    flip_ref[...] = jnp.transpose(gate_ref[...])

    def heads_of(ref, step):
        tiles = [ref[pl.ds(starts[step], BLK), pl.ds(g * 128, 128)] for g in range(3)]
        zero = jnp.zeros_like(tiles[0])
        return jnp.concatenate(
            [jnp.where(low, t, zero) for t in tiles] + [jnp.where(low, zero, t) for t in tiles],
            axis=0,
        )

    def score(step):
        return (
            dot_t(heads_of(plain_ref, step), sk[...]),
            dot_t(heads_of(turned_ref, step), kg[step]),
        )

    def finish(step, coarse, fine):
        own = (index * 8 + blocks[step]) * BLK
        coarse = jnp.where(limit_ref[...] <= own, coarse, NEG)
        peak = jnp.maximum(jnp.max(coarse, axis=-1, keepdims=True), NEG * 0.01)
        powers = jnp.exp(coarse - peak)
        total = jnp.maximum(jnp.sum(powers, axis=-1, keepdims=True), 1.0)
        coarse_out = dot((powers * (1.0 / total)).astype(BF), sv[...])

        fine = fine + bias_ref[pl.ds(blocks[step], 1), :]
        fine = jnp.concatenate([fine[:, :128] + triangle, fine[:, 128:]], axis=1)
        fine_powers = jnp.exp(fine - jnp.max(fine, axis=-1, keepdims=True))
        inverse = 1.0 / jnp.sum(fine_powers, axis=-1, keepdims=True)
        fine_out = dot(fine_powers.astype(BF), vg[step])

        gates = flip_ref[pl.ds(starts[step], BLK), :]
        target = send_ref if step < 4 else keep_ref
        for g in range(3):
            a, b = g * BLK, (3 + g) * BLK
            gate = jnp.where(low, gates[:, g : g + 1], gates[:, 3 + g : 4 + g])
            fine_gate = jnp.where(
                low,
                gates[:, 8 + g : 9 + g] * inverse[a : a + BLK],
                gates[:, 11 + g : 12 + g] * inverse[b : b + BLK],
            )
            mixed = gate * jnp.where(low, coarse_out[a : a + BLK], coarse_out[b : b + BLK])
            mixed += fine_gate * jnp.where(low, fine_out[a : a + BLK], fine_out[b : b + BLK])
            target[pl.ds((step % 4) * BLK, BLK), pl.ds(g * 128, 128)] = mixed.astype(BF)

    ahead = score(0)
    for step in range(8):
        now, ahead = ahead, score(step + 1) if step < 7 else None
        finish(step, *now)


def by_group(mixed_ref, weight_ref):
    total = None
    for g in range(3):
        weight = jnp.concatenate(
            [weight_ref[pl.ds(g * HEAD, HEAD), :], weight_ref[pl.ds((3 + g) * HEAD, HEAD), :]],
            axis=0,
        )
        part = dot(mixed_ref[:, pl.ds(g * 128, 128)], weight)
        total = part if total is None else total + part
    return total


def kept_kernel(keep_ref, weight_ref, out_ref):
    out_ref[...] = by_group(keep_ref, weight_ref)


def out_kernel(part_ref, got_ref, weight_ref, gain_ref, out_ref):
    summed = part_ref[...] + by_group(got_ref, weight_ref)
    mean = jnp.mean(summed * summed, axis=-1, keepdims=True)
    out_ref[...] = summed * lax.rsqrt(mean + EPS) * gain_ref[...]


VMEM = pl.BlockSpec(memory_space=pltpu.VMEM)
HBM = pl.BlockSpec(memory_space=pltpu.HBM)
SMEM = pl.BlockSpec(memory_space=pltpu.SMEM)


def call(kernel, out_shape, specs, args, scratch=(), flops=0, data=0, vmem=12 * 2**20):
    return pl.pallas_call(
        kernel,
        out_shape=out_shape,
        in_specs=specs,
        out_specs=jax.tree.map(lambda _: VMEM, out_shape),
        scratch_shapes=scratch,
        compiler_params=pltpu.CompilerParams(vmem_limit_bytes=vmem),
        cost_estimate=pl.CostEstimate(flops=flops, bytes_accessed=data, transcendentals=0),
    )(*args)


def z_shift(d):
    return [(z * Y + y, (z + d) % Z * Y + y) for z in range(Z) for y in range(Y)]


def y_shift(d):
    return [(z * Y + y, z * Y + (y + d) % Y) for z in range(Z) for y in range(Y)]


def z_pair():
    return [(z * Y + y, (z ^ 1) * Y + y) for z in range(Z) for y in range(Y)]


def pair_groups():
    return [[(2 * p + a) * Y + y for a in range(2) for y in range(Y)] for p in range(Z // 2)]


def rope_tables(positions):
    half = HEAD // 2
    inverse = ROPE_BASE ** (-jnp.arange(half, dtype=F32) * (2.0 / HEAD))
    angles = positions.astype(F32)[:, None] * inverse[None, :]
    cosine, sine = jnp.cos(angles), jnp.sin(angles)
    return (
        jnp.concatenate([cosine] * 4, axis=-1),
        jnp.concatenate([-sine, sine, -sine, sine], axis=-1),
    )


def on_device(
    tokens,
    query_weight,
    key_weight,
    value_weight,
    gate_weight,
    compress_weight,
    out_weight,
    out_gain,
    chosen,
):
    shape = jax.ShapeDtypeStruct
    x = tokens[0]
    index = lax.axis_index("kv")
    other_weight = lax.ppermute(out_weight, "tp", [(0, 1), (1, 0)])
    ask = call(
        ask_kernel, shape((8, 128), jnp.int32), [VMEM], (chosen[0],), flops=2**32, data=2**12
    )
    partner_ask = lax.ppermute(ask, "kv", z_pair())

    cosine, sine = rope_tables(index * 256 + jnp.arange(256, dtype=jnp.int32))
    unit = call(
        kv_kernel,
        shape((UNIT, 128), BF),
        [VMEM] * 7,
        (ask, x, key_weight, value_weight, compress_weight, cosine, sine),
        flops=2 * 256 * 2048 * 256,
        data=2 * 2**20,
    )
    units = [unit] + [lax.ppermute(unit, "kv", z_shift(d)) for d in (2, 4, 6)]
    asks = jnp.concatenate([ask, partner_ask])
    asks = [asks] + [lax.ppermute(asks, "kv", y_shift(-d)) for d in (1, 2, 3)]

    plain, turned, gates, rows, bias = call(
        q_kernel,
        (
            shape((256, 384), BF),
            shape((256, 384), BF),
            shape((16, 256), F32),
            shape((8, TOPN), jnp.int32),
            shape((8, TOPN * BLK), F32),
        ),
        [SMEM] + [VMEM] * 6,
        (chosen[0], chosen[0], x, query_weight, gate_weight.T, cosine, sine),
        flops=2 * 256 * 2048 * 408,
        data=3 * 2**20,
    )
    share = call(
        select_kernel,
        shape((8 * SHARE, 128), BF),
        [SMEM] * 4 + [VMEM] * 4,
        (*asks, *units),
        flops=2**20,
        data=2 * 2**20,
    )
    pool = lax.all_to_all(
        share.reshape(8, SHARE, 128), "kv", 0, 0, tiled=True, axis_index_groups=pair_groups()
    ).reshape(8 * SHARE, 128)

    keep, send = call(
        attend_kernel,
        (shape((128, 384), BF), shape((128, 384), BF)),
        [SMEM] + [VMEM] * 6,
        (rows, bias, plain, turned, gates, unit, pool),
        scratch=[
            pltpu.VMEM((256, 128), BF),
            pltpu.VMEM((256, 128), BF),
            pltpu.VMEM((8, 512, 128), BF),
            pltpu.VMEM((8, 512, 128), BF),
            pltpu.VMEM((192, 256), jnp.int32),
            pltpu.VMEM((256, 16), F32),
        ],
        flops=2**30,
        data=4 * 2**20,
        vmem=12 * 2**20,
    )
    got = lax.ppermute(send, "tp", [(0, 1), (1, 0)])
    part = call(
        kept_kernel,
        shape((128, 2048), F32),
        [VMEM] * 2,
        (keep, out_weight),
        flops=2 * 128 * 384 * 2048,
        data=3 * 2**20,
    )
    out = call(
        out_kernel,
        shape((128, 2048), F32),
        [VMEM] * 4,
        (part, got, other_weight, out_gain[None]),
        flops=2 * 128 * 384 * 2048,
        data=4 * 2**20,
    )
    return out[None]


def solution(mesh):
    in_specs = (
        P("dp", "kv", None),
        P(None, "tp"),
        P(None, "tp"),
        P(None, "tp"),
        P(),
        P(),
        P("tp", None),
        P(),
        P("dp", "kv", None),
    )
    out_specs = P("dp", ("kv", "tp"), None)

    return jax.shard_map(
        on_device, mesh=mesh, in_specs=in_specs, out_specs=out_specs, check_vma=False
    )
```

```python
import jax
import jax.numpy as jnp
from jax import lax
from jax.experimental import pallas as pl
from jax.experimental.pallas import tpu as pltpu
from jax.sharding import PartitionSpec as P


HEAD = 64
BLK = 32
TOPN = 16
NEG = -1e30
ROPE_BASE = 500000.0
EPS = 1e-06
Z, Y = 8, 4
UNIT = 528
SHARE = 576
PIECE = 144
BF = jnp.bfloat16
F32 = jnp.float32


def dot(a, b):
    return jnp.dot(a, b, preferred_element_type=F32)


def dot_t(a, b):
    return lax.dot_general(a, b, (((1,), (1,)), ((), ())), preferred_element_type=F32)


def turn(x, cosine, sine):
    lane = lax.broadcasted_iota(jnp.int32, x.shape, 1)
    other = jnp.where(lane % HEAD < HEAD // 2, pltpu.roll(x, 96, 1), pltpu.roll(x, 32, 1))
    return x * cosine + other * sine


def kv_kernel(after_ref, x_ref, wk_ref, wv_ref, cw_ref, cos_ref, sin_ref, out_ref):
    x = x_ref[...]
    keys = dot(x, wk_ref[...]).astype(BF).astype(F32)
    out_ref[pl.ds(0, 256), :] = turn(keys, cos_ref[...], sin_ref[...]).astype(BF)
    values = dot(x, wv_ref[...]).astype(BF)
    out_ref[pl.ds(256, 256), :] = values

    def compress(rows, weight):
        wide = jnp.concatenate([weight, weight], axis=1)
        return jnp.sum(rows.reshape(8, BLK, 128) * wide[None], axis=1)

    packed = jnp.concatenate(
        [compress(keys, cw_ref[0]), compress(values.astype(F32), cw_ref[1])], axis=0
    )
    out_ref[pl.ds(512, 16), :] = packed.astype(BF)


def ask_kernel(listed_ref, ask_ref):
    listed = listed_ref[...]
    lane = lax.broadcasted_iota(jnp.int32, (8, 128), 1)
    low, high = jnp.full((8, 128), 7, jnp.int32), jnp.zeros((8, 128), jnp.int32)
    for t in range(TOPN):
        entry = jnp.broadcast_to(listed[:, t : t + 1], (8, 128))
        hit = (entry >> 3) == lane
        low = jnp.minimum(low, jnp.where(hit, entry & 7, 7))
        high = jnp.maximum(high, jnp.where(hit, entry & 7, 0))
    low = jnp.min(low, axis=0, keepdims=True)
    high = jnp.max(high, axis=0, keepdims=True)
    first = lax.broadcasted_iota(jnp.int32, (8, 128), 0) == 0
    ask_ref[...] = jnp.where(first, low, high)


def fill_tables(scalar_ref, listed, rows_ref, bias_ref):
    index = lax.axis_index("kv")
    z, y = index // Y, index % Y
    lane = lax.broadcasted_iota(jnp.int32, (8, 128), 1)
    for g in range(4):
        row = jnp.zeros((8, 128), F32)
        for part in range(4):
            entry = jnp.broadcast_to(listed[:, g * 4 + part : g * 4 + part + 1], (8, 128))
            row = jnp.where((lane >> 5) == part, jnp.where(entry >= 0, 0.0, NEG), row)
        bias_ref[:, pl.ds(g * 128, 128)] = row
    owner = listed >> 3
    second = jnp.zeros((8, TOPN), jnp.int32)
    for i in range(8):
        for t in range(TOPN):
            other = scalar_ref[i, t]
            second = jnp.where((owner == (other >> 3)) & (other < listed), 1, second)
    owner = jnp.maximum(listed, 0) >> 3
    owner_z = owner >> 2
    other = (owner_z ^ z) & 1
    sender = other * Y + ((owner & 3) ^ y)
    u = (((z ^ other) - owner_z) & 7) >> 1
    rows_ref[...] = sender * SHARE + u * PIECE + second * BLK


def q_kernel(scalar_ref, listed_ref, x_ref, wq_ref, wg_ref, cos_ref, sin_ref, *outs):
    plain_ref, turned_ref, gate_ref, rows_ref, bias_ref = outs
    fill_tables(scalar_ref, listed_ref[...], rows_ref, bias_ref)
    x = x_ref[...]
    logits = dot_t(wg_ref[...], x)
    first_core = lax.axis_index("tp") == 0
    for branch in range(2):
        at = branch * 12
        own = jnp.where(first_core, logits[at : at + 6], logits[at + 6 : at + 12])
        gate_ref[branch * 8 : branch * 8 + 6, :] = jax.nn.sigmoid(own)
    lane = lax.broadcasted_iota(jnp.int32, (256, 128), 1)
    plain, turned = [], []
    for pair in range(3):
        q = dot(x, wq_ref[:, pl.ds(pair * 128, 128)]).astype(BF).astype(F32)
        plain.append(q * 0.125)
        turned.append(turn(q, cos_ref[...], sin_ref[...]).astype(BF).astype(F32) * 0.125)
    for tiles, out in ((plain, plain_ref), (turned, turned_ref)):
        groups = (
            jnp.where(lane < HEAD, tiles[0], tiles[1]),
            jnp.where(lane < HEAD, pltpu.roll(tiles[0], 64, 1), pltpu.roll(tiles[2], 64, 1)),
            jnp.where(lane < HEAD, tiles[1], tiles[2]),
        )
        for g in range(3):
            out[:, pl.ds(g * 128, 128)] = groups[g].astype(BF)


def select_kernel(*refs):
    asks, units, outs = refs[:Y], refs[Y : Y + 4], refs[Y + 4 :]
    index = lax.axis_index("kv")
    z, y = index // Y, index % Y
    for partner in range(2):
        for d in range(Y):
            out = outs[partner * Y + d]
            for u in range(4):
                base = u * PIECE
                source = lax.rem(z - 2 * u + Z, Z) * Y + y
                for slot in range(2):
                    row = pl.multiple_of(asks[d][partner * 8 + slot, source] * BLK, BLK)
                    at = base + slot * BLK
                    out[pl.ds(at, BLK), :] = units[u][pl.ds(row, BLK), :]
                    out[pl.ds(at + 64, BLK), :] = units[u][pl.ds(row + 256, BLK), :]
                out[pl.ds(base + 128, 16), :] = units[u][pl.ds(512, 16), :]


def attend_kernel(
    row_ref, bias_ref, plain_ref, turned_ref, gate_ref, unit_ref, *refs
):
    shares = refs[:8]
    keep_ref, send_ref, pool, sk, sv, kg, vg, limit_ref, flip_ref = refs[8:]
    index = lax.axis_index("kv")
    z, y, core = index // Y, index % Y, lax.axis_index("tp")
    blocks = [lax.rem(step + 4 * (1 - core), 8) for step in range(8)]
    starts = [pl.multiple_of(i * BLK, BLK) for i in blocks]
    for piece in range(32):
        share, base = shares[piece // 4], piece % 4 * PIECE
        pool[pl.ds(piece * PIECE, 128), :] = share[pl.ds(base, 128), :]
        sk[pl.ds(piece * 8, 8), :] = share[pl.ds(base + 128, 8), :]
        sv[pl.ds(piece * 8, 8), :] = share[pl.ds(base + 136, 8), :]
    for step in range(8):
        kg[step, pl.ds(0, BLK), :] = unit_ref[pl.ds(starts[step], BLK), :]
        vg[step, pl.ds(0, BLK), :] = unit_ref[pl.ds(starts[step] + 256, BLK), :]
        for t in range(1, TOPN):
            at = pl.multiple_of(row_ref[blocks[step], t], 16)
            kg[step, pl.ds(t * BLK, BLK), :] = pool[pl.ds(at, BLK), :]
            vg[step, pl.ds(t * BLK, BLK), :] = pool[pl.ds(at + 64, BLK), :]

    column = lax.broadcasted_iota(jnp.int32, (192, 256), 1)
    row = lax.broadcasted_iota(jnp.int32, (192, 256), 0) % BLK
    owner_z = ((z ^ (column // 128)) - 2 * (column // 8 % 4) + Z) % Z
    dev = owner_z * Y + (y ^ (column // 32 % Y))
    limit_ref[...] = (dev * 8 + column % 8) * BLK + (BLK - 1) - row
    triangle = jnp.where(
        (column[:, :128] < BLK) & (column[:, :128] > row[:, :128]), NEG, 0.0
    )
    lane = lax.broadcasted_iota(jnp.int32, (BLK, 128), 1)
    low = lane < HEAD
    flip_ref[...] = jnp.transpose(gate_ref[...])

    def heads_of(ref, step):
        tiles = [ref[pl.ds(starts[step], BLK), pl.ds(g * 128, 128)] for g in range(3)]
        zero = jnp.zeros_like(tiles[0])
        return jnp.concatenate(
            [jnp.where(low, t, zero) for t in tiles] + [jnp.where(low, zero, t) for t in tiles],
            axis=0,
        )

    def score(step):
        return (
            dot_t(heads_of(plain_ref, step), sk[...]),
            dot_t(heads_of(turned_ref, step), kg[step]),
        )

    def finish(step, coarse, fine):
        own = (index * 8 + blocks[step]) * BLK
        coarse = jnp.where(limit_ref[...] <= own, coarse, NEG)
        peak = jnp.maximum(jnp.max(coarse, axis=-1, keepdims=True), NEG * 0.01)
        powers = jnp.exp(coarse - peak)
        total = jnp.maximum(jnp.sum(powers, axis=-1, keepdims=True), 1.0)
        coarse_out = dot((powers * (1.0 / total)).astype(BF), sv[...])

        fine = fine + bias_ref[pl.ds(blocks[step], 1), :]
        fine = jnp.concatenate([fine[:, :128] + triangle, fine[:, 128:]], axis=1)
        fine_powers = jnp.exp(fine - jnp.max(fine, axis=-1, keepdims=True))
        inverse = 1.0 / jnp.sum(fine_powers, axis=-1, keepdims=True)
        fine_out = dot(fine_powers.astype(BF), vg[step])

        gates = flip_ref[pl.ds(starts[step], BLK), :]
        target = send_ref if step < 4 else keep_ref
        for g in range(3):
            a, b = g * BLK, (3 + g) * BLK
            gate = jnp.where(low, gates[:, g : g + 1], gates[:, 3 + g : 4 + g])
            fine_gate = jnp.where(
                low,
                gates[:, 8 + g : 9 + g] * inverse[a : a + BLK],
                gates[:, 11 + g : 12 + g] * inverse[b : b + BLK],
            )
            mixed = gate * jnp.where(low, coarse_out[a : a + BLK], coarse_out[b : b + BLK])
            mixed += fine_gate * jnp.where(low, fine_out[a : a + BLK], fine_out[b : b + BLK])
            target[pl.ds((step % 4) * BLK, BLK), pl.ds(g * 128, 128)] = mixed.astype(BF)

    ahead = score(0)
    for step in range(8):
        now, ahead = ahead, score(step + 1) if step < 7 else None
        finish(step, *now)


def by_group(mixed_ref, weight_ref):
    total = None
    for g in range(3):
        weight = jnp.concatenate(
            [weight_ref[pl.ds(g * HEAD, HEAD), :], weight_ref[pl.ds((3 + g) * HEAD, HEAD), :]],
            axis=0,
        )
        part = dot(mixed_ref[:, pl.ds(g * 128, 128)], weight)
        total = part if total is None else total + part
    return total


def kept_kernel(keep_ref, weight_ref, out_ref):
    out_ref[...] = by_group(keep_ref, weight_ref)


def out_kernel(part_ref, got_ref, weight_ref, gain_ref, out_ref):
    summed = part_ref[...] + by_group(got_ref, weight_ref)
    mean = jnp.mean(summed * summed, axis=-1, keepdims=True)
    out_ref[...] = summed * lax.rsqrt(mean + EPS) * gain_ref[...]


VMEM = pl.BlockSpec(memory_space=pltpu.VMEM)
HBM = pl.BlockSpec(memory_space=pltpu.HBM)
SMEM = pl.BlockSpec(memory_space=pltpu.SMEM)


def call(kernel, out_shape, specs, args, scratch=(), flops=0, data=0, vmem=12 * 2**20):
    return pl.pallas_call(
        kernel,
        out_shape=out_shape,
        in_specs=specs,
        out_specs=jax.tree.map(lambda _: VMEM, out_shape),
        scratch_shapes=scratch,
        compiler_params=pltpu.CompilerParams(vmem_limit_bytes=vmem),
        cost_estimate=pl.CostEstimate(flops=flops, bytes_accessed=data, transcendentals=0),
    )(*args)


def shift(dz):
    return [(z * Y + y, (z + dz) % Z * Y + y) for z in range(Z) for y in range(Y)]


def swap(dz, dy):
    return [(z * Y + y, (z ^ dz) * Y + (y ^ dy)) for z in range(Z) for y in range(Y)]


def rope_tables(positions):
    half = HEAD // 2
    inverse = ROPE_BASE ** (-jnp.arange(half, dtype=F32) * (2.0 / HEAD))
    angles = positions.astype(F32)[:, None] * inverse[None, :]
    cosine, sine = jnp.cos(angles), jnp.sin(angles)
    return (
        jnp.concatenate([cosine] * 4, axis=-1),
        jnp.concatenate([-sine, sine, -sine, sine], axis=-1),
    )


def on_device(
    tokens,
    query_weight,
    key_weight,
    value_weight,
    gate_weight,
    compress_weight,
    out_weight,
    out_gain,
    chosen,
):
    shape = jax.ShapeDtypeStruct
    x = tokens[0]
    index = lax.axis_index("kv")
    ask = call(
        ask_kernel, shape((8, 128), jnp.int32), [VMEM], (chosen[0],), flops=2**32, data=2**12
    )
    partner_ask = lax.ppermute(ask, "kv", swap(1, 0))

    cosine, sine = rope_tables(index * 256 + jnp.arange(256, dtype=jnp.int32))
    unit = call(
        kv_kernel,
        shape((UNIT, 128), BF),
        [VMEM] * 7,
        (ask, x, key_weight, value_weight, compress_weight, cosine, sine),
        flops=2 * 256 * 2048 * 256,
        data=2 * 2**20,
    )
    units = [unit] + [lax.ppermute(unit, "kv", shift(dz)) for dz in (2, 4, 6)]
    asks = jnp.concatenate([ask, partner_ask])
    asks = [asks] + [lax.ppermute(asks, "kv", swap(0, dy)) for dy in (1, 2, 3)]

    plain, turned, gates, rows, bias = call(
        q_kernel,
        (
            shape((256, 384), BF),
            shape((256, 384), BF),
            shape((16, 256), F32),
            shape((8, TOPN), jnp.int32),
            shape((8, TOPN * BLK), F32),
        ),
        [SMEM] + [VMEM] * 6,
        (chosen[0], chosen[0], x, query_weight, gate_weight.T, cosine, sine),
        flops=2 * 256 * 2048 * 408,
        data=3 * 2**20,
    )
    shares = call(
        select_kernel,
        (shape((SHARE, 128), BF),) * 8,
        [SMEM] * 4 + [VMEM] * 4,
        (*asks, *units),
        flops=2**20,
        data=2 * 2**20,
    )
    shares = list(shares)
    shares[0], other_weight = lax.optimization_barrier((shares[0], out_weight))
    other_weight = lax.ppermute(other_weight, "tp", [(0, 1), (1, 0)])
    for dz, dy in ((0, 2), (1, 1), (1, 3), (0, 1), (0, 3), (1, 2), (1, 0)):
        k = dz * Y + dy
        shares[k] = lax.ppermute(shares[k], "kv", swap(dz, dy))

    keep, send = call(
        attend_kernel,
        (shape((128, 384), BF), shape((128, 384), BF)),
        [SMEM] + [VMEM] * 13,
        (rows, bias, plain, turned, gates, unit, *shares),
        scratch=[
            pltpu.VMEM((8 * SHARE, 128), BF),
            pltpu.VMEM((256, 128), BF),
            pltpu.VMEM((256, 128), BF),
            pltpu.VMEM((8, 512, 128), BF),
            pltpu.VMEM((8, 512, 128), BF),
            pltpu.VMEM((192, 256), jnp.int32),
            pltpu.VMEM((256, 16), F32),
        ],
        flops=2**30,
        data=4 * 2**20,
        vmem=12 * 2**20,
    )
    got = lax.ppermute(send, "tp", [(0, 1), (1, 0)])
    part = call(
        kept_kernel,
        shape((128, 2048), F32),
        [VMEM] * 2,
        (keep, out_weight),
        flops=2 * 128 * 384 * 2048,
        data=3 * 2**20,
    )
    out = call(
        out_kernel,
        shape((128, 2048), F32),
        [VMEM] * 4,
        (part, got, other_weight, out_gain[None]),
        flops=2 * 128 * 384 * 2048,
        data=4 * 2**20,
    )
    return out[None]


def solution(mesh):
    in_specs = (
        P("dp", "kv", None),
        P(None, "tp"),
        P(None, "tp"),
        P(None, "tp"),
        P(),
        P(),
        P("tp", None),
        P(),
        P("dp", "kv", None),
    )
    out_specs = P("dp", ("kv", "tp"), None)

    return jax.shard_map(
        on_device, mesh=mesh, in_specs=in_specs, out_specs=out_specs, check_vma=False
    )
```
